512 devices in a mesh: grp: 2 (over y), sp: 16 (over z), dp: 16 (over x, core).
Axes of the slice: x: 8, y: 2, z: 16, core: 2. Of those that a mesh axis runs over, the one named last changes fastest.
The devices are a block of a 8x8x16 slice.
Arguments:
- query_rows: bfloat16 [32, 2048, 2048], P(('grp', 'dp'), 'sp'), parts along dimension 0, may hold values from -6 to 6
- key_rows: bfloat16 [32, 2048, 2048], P(('grp', 'dp'), 'sp'), parts along dimension 0, may hold values from -6 to 6
- value_rows: bfloat16 [32, 2048, 2048], P(('grp', 'dp'), 'sp'), parts along dimension 0, may hold values from -6 to 6
- query_gain: float32 [64], replicated, may hold values from 1.1 to 7
- key_gain: float32 [64], replicated, may hold values from 1.1 to 7
- lambdas: float32 [16], replicated, may hold values from 0.3 to 0.8
- head_gain: float32 [128], replicated, may hold values from 0.1 to 1.9
- out_weight: bfloat16 [2048, 2048], P(None, 'dp'), may hold values from -0.125 to 0.125
Outputs:
- attended: bfloat16 [32, 2048, 2048], P(('grp', 'dp'), 'sp'), parts along dimension 0
The draws below stay inside these ranges and needn't reach their ends.
There are 2 independent parts, one for each index of `grp`. The reference program is written for one: setup_inputs(seed, part) draws one part's arguments, and reference() takes and returns one part's arrays. A program takes and returns all parts, laid end to end along the dimension named above; an argument that names none is the same for every part. Nothing has to cross between parts.
All inputs are finite; a program needn't handle non-finite values.
Results may differ from the reference program's by a relative error of at most 0.008.
The reference program's roundings to bfloat16 on the way count: a program that leaves them out, or rounds other values in their place, can miss the bound.
Values may be sent and summed in bfloat16 or wider, within the bound.
A program may use at most 128 MiB of HBM per device.

```python
import jax
import jax.numpy as jnp
from jax import lax

D = 2048
HEADS = 16
HEAD = 64
VDIM = 128
LENGTH = 2048
SEQS = 16


def paired_rows(key):
    shape = (SEQS, LENGTH, HEADS * 2 * HEAD)
    key_part = jnp.clip(jax.random.normal(jax.random.fold_in(key, 101), shape, jnp.float32), -6.0, 6.0)
    query_part = jnp.clip(jax.random.normal(jax.random.fold_in(key, 202), shape, jnp.float32), -6.0, 6.0)
    return (query_part, key_part)


def draw_query_rows(key, part):
    return paired_rows(key)[0].astype(jnp.bfloat16)


def draw_key_rows(key, part):
    return paired_rows(key)[1].astype(jnp.bfloat16)


def gain_draw(key):
    return jax.random.uniform(key, (HEAD,), jnp.float32, 1.1, 1.7)


def draw_query_gain(key, part):
    return gain_draw(jax.random.fold_in(key, 31))


def draw_key_gain(key, part):
    return gain_draw(jax.random.fold_in(key, 32))


def shard_levels(key, shape, cuts, smallest, largest):
    level, own = 1.0, jax.random.fold_in(key, 6)
    for dim, shards_of in cuts:
        steps = jnp.exp(jax.random.uniform(jax.random.fold_in(own, dim), (shards_of,), jnp.float32, smallest / len(cuts), largest / len(cuts)))
        level = level * jnp.repeat(steps, shape[dim] // shards_of).reshape([-1 if axis == dim else 1 for axis in range(len(shape))])
    return level


def noise(rng, shape, scale, limit, split=(), kind=jnp.bfloat16):
    factor_of = shard_levels(rng, shape, split, -0.22, 0.18) if split else 1.0
    values = jax.random.normal(rng, shape, jnp.float32) * scale * factor_of
    return jnp.minimum(jnp.maximum(values, -limit), limit).astype(kind)


def setup_inputs(seed: int = 0, part: int = 0) -> dict:
    key_of = jax.random.split(jax.random.key(seed), 9)
    own_keys = jax.random.split(jax.random.fold_in(key_of[8], part), 9)
    query_rows = draw_query_rows(jax.random.fold_in(jax.random.fold_in(key_of[8], part), 71), part)
    key_rows = draw_key_rows(jax.random.fold_in(jax.random.fold_in(key_of[8], part), 71), part)
    value_rows = noise(own_keys[2], (SEQS, LENGTH, HEADS * VDIM), 1.0, 6.0, ((0, 16), (1, 16)))
    query_gain = draw_query_gain(jax.random.fold_in(key_of[8], 71), part)
    key_gain = draw_key_gain(jax.random.fold_in(key_of[8], 71), part)
    lambdas = jnp.clip(jax.random.uniform(key_of[5], (HEADS,), jnp.float32, 0.3, 0.8), 0.3, 0.8)
    head_gain = jnp.clip(1.0 + 0.18 * jax.random.normal(key_of[6], (VDIM,), jnp.float32), 0.1, 1.9)
    out_weight = noise(key_of[7], (HEADS * VDIM, D), (HEADS * VDIM) ** -0.5, 0.125, ((1, 16),))
    return {"query_rows": query_rows, "key_rows": key_rows, "value_rows": value_rows, "query_gain": query_gain, "key_gain": key_gain, "lambdas": lambdas, "head_gain": head_gain, "out_weight": out_weight}


EPSILON = 1e-06
OUT_SCALE = 0.8

def norm_rotate(field_rows, gain_vector, positions):
    widened = field_rows.astype(jnp.float32)
    normed = widened * lax.rsqrt(lax.optimization_barrier(jnp.mean(widened * widened, axis=-1, keepdims=True)) + EPSILON) * gain_vector
    half_size = field_rows.shape[-1] // 2
    inverse = 10000.0 ** (-jnp.arange(half_size, dtype=jnp.float32) / half_size)
    angles = (positions[:, None] * inverse[None, :]).reshape(positions.shape[0], 1, 1, half_size)
    cosine_part = jnp.cos(angles)
    sine_part = jnp.sin(angles)
    first_half = normed[..., :half_size]
    second_half = normed[..., half_size:]
    turned = jnp.concatenate([first_half * cosine_part - second_half * sine_part, second_half * cosine_part + first_half * sine_part], axis=-1)
    return turned.astype(jnp.bfloat16)

def head_norm(raw_heads, gain_vector):
    scaled = raw_heads * lax.rsqrt(lax.optimization_barrier(jnp.mean(raw_heads * raw_heads, axis=-1, keepdims=True)) + EPSILON)
    return (scaled * gain_vector * OUT_SCALE).astype(jnp.bfloat16)

def block_size(length):
    return 512 if length % 512 == 0 else length

def attend(query_head, key_head, value_head, weight_two, gain_vector):
    length = query_head.shape[0]
    block_rows = block_size(length)
    score_scale = query_head.shape[-1] ** (-0.5)
    key_wide = key_head.astype(jnp.float32)
    key_positions = jnp.arange(length, dtype=jnp.int32)

    def one_block(number):
        first_row = number * block_rows
        query_block = lax.dynamic_slice_in_dim(query_head, first_row, block_rows, 0).astype(jnp.float32)
        scores = jnp.einsum('qcd,kcd->cqk', query_block, key_wide) * score_scale
        query_positions = first_row + jnp.arange(block_rows, dtype=jnp.int32)
        visible = key_positions[None, :] <= query_positions[:, None]
        scores = jnp.where(visible[None], scores, -1e+30)
        highest = lax.optimization_barrier(jnp.max(scores, axis=-1, keepdims=True))
        exponent = jnp.exp(scores - highest)
        probabilities = exponent / lax.optimization_barrier(jnp.sum(exponent, axis=-1, keepdims=True))
        mixing = (probabilities[0] - weight_two * probabilities[1]).astype(jnp.bfloat16)
        return jnp.dot(mixing, value_head, preferred_element_type=jnp.float32)
    blocks = lax.map(one_block, jnp.arange(length // block_rows, dtype=jnp.int32))
    return head_norm(blocks.reshape(length, value_head.shape[-1]), gain_vector)

def reference(query_rows, key_rows, value_rows, query_gain, key_gain, lambdas, head_gain, out_weight):
    seq_count = query_rows.shape[0]
    length = query_rows.shape[1]
    positions = jnp.arange(length, dtype=jnp.float32)
    query_rot = norm_rotate(query_rows.reshape(seq_count, length, HEADS, 2, HEAD), query_gain, positions)
    key_rot = norm_rotate(key_rows.reshape(seq_count, length, HEADS, 2, HEAD), key_gain, positions)
    value_heads = value_rows.reshape(seq_count, length, HEADS, VDIM)

    def per_item(number):
        seq_index = number // HEADS
        head_index = number % HEADS
        return attend(query_rot[seq_index, :, head_index], key_rot[seq_index, :, head_index], value_heads[seq_index, :, head_index], lambdas[head_index], head_gain)
    outputs = lax.map(per_item, jnp.arange(seq_count * HEADS, dtype=jnp.int32))
    outputs = outputs.reshape(seq_count, HEADS, length, VDIM).transpose(0, 2, 1, 3)
    outputs = outputs.reshape(seq_count * length, HEADS * VDIM)
    attended = jnp.dot(outputs, out_weight, preferred_element_type=jnp.float32).astype(jnp.bfloat16)
    return attended.reshape(seq_count, length, out_weight.shape[1])
```

```python
import functools

import jax
import jax.numpy as jnp
import numpy as np
from jax import lax
from jax.experimental import pallas as pl
from jax.experimental.pallas import tpu as pltpu
from jax.sharding import PartitionSpec as P

EPSILON = 1e-06
OUT_SCALE = 0.8
LOG2E = 1.4426950408889634
NEG = -1e30
MESH = pl.DeviceIdType.MESH
CHUNK = 4


def rope_tables(blocks, block, head):
    half = head // 2
    lane = np.arange(2 * head) % head
    inverse = 10000.0 ** (-(lane % half).astype(np.float64) / half)
    sign = np.where(lane < half, -1.0, 1.0)

    def pair(positions):
        angle = positions[:, None] * inverse[None, :]
        return np.stack([np.cos(angle), sign * np.sin(angle)]).astype(np.float32)

    return pair(np.arange(blocks) * float(block)), pair(np.arange(block).astype(np.float64))


def kernel(
    n, nd, head,
    q_hbm, k_hbm, v_hbm, w_hbm, qg_ref, kg_ref, lam_ref, hg_ref, base_ref, offs_ref,
    out_ref,
    kraw, qraw, krot, vall, osend, oin, w_all, sc, acc, gains,
    loc_sem, send_sem, recv_sem, wsend, wrecv, psend, precv,
):
    me = lax.axis_index("sp")
    dp = lax.axis_index("dp")
    core = lax.rem(dp, 2)
    partner = dp + 1 - 2 * core
    right, left = lax.rem(dp + 2, nd), lax.rem(dp + nd - 2, nd)
    steps = nd // 4
    tok = out_ref.shape[1]
    depth, width = w_hbm.shape
    lanes = 2 * head

    def peer_of(t):
        d = (t + 1) // 2
        return lax.rem(me + jnp.where(lax.rem(t, 2) == 1, d, n - d), n)

    def barrier():
        sem = pltpu.get_barrier_semaphore()

        def tell(t, c):
            pl.semaphore_signal(sem, inc=1, device_id={"sp": peer_of(t)}, device_id_type=MESH)
            return c

        lax.fori_loop(1, n, tell, 0)
        for d in (right, left, partner):
            pl.semaphore_signal(sem, inc=1, device_id={"dp": d}, device_id_type=MESH)
        pl.semaphore_wait(sem, n + 2)

    def chunk_copy(which, t):
        peer = peer_of(t)
        if which == 3:
            src, dst = osend.at[peer], oin.at[me]
        else:
            hbm = (k_hbm, v_hbm, q_hbm)[which]
            src = hbm.at[0, :, pl.ds(pl.multiple_of(peer * lanes, lanes), lanes)]
            if which == 1:
                dst = vall.at[pl.ds(pl.multiple_of(me * tok, tok), tok), :]
            else:
                dst = (kraw if which == 0 else qraw).at[me]
        return pltpu.make_async_remote_copy(
            src_ref=src, dst_ref=dst,
            send_sem=send_sem.at[which, t], recv_sem=recv_sem.at[which, me],
            device_id={"sp": peer}, device_id_type=MESH,
        )

    def chunk_arrived(which, t):
        peer = peer_of(t)
        if which == 1:
            dst = vall.at[pl.ds(pl.multiple_of(peer * tok, tok), tok), :]
        else:
            dst = (kraw, None, qraw, oin)[which].at[peer]
        pltpu.make_async_remote_copy(
            src_ref=dst, dst_ref=dst,
            send_sem=send_sem.at[which, t], recv_sem=recv_sem.at[which, peer],
            device_id={"sp": peer}, device_id_type=MESH,
        ).wait_recv()

    def start_all(which):
        def go(t, c):
            chunk_copy(which, t).start()
            return c

        lax.fori_loop(1, n, go, 0)

    def start_far(which):
        def go(s, c):
            chunk_copy(which, n - s).start()
            return c

        lax.fori_loop(1, n, go, 0)

    def own(which):
        cols = pl.ds(pl.multiple_of(me * lanes, lanes), lanes)
        hbm = (k_hbm, v_hbm, q_hbm)[which]
        if which == 1:
            dst = vall.at[pl.ds(pl.multiple_of(me * tok, tok), tok), :]
        else:
            dst = (kraw if which == 0 else qraw).at[me]
        return pltpu.make_async_copy(hbm.at[0, :, cols], dst, loc_sem.at[which])

    def w_at(owner, lo=0, rows=None):
        rows = depth if rows is None else rows
        return w_all.at[pl.ds(lo, rows), pl.ds(pl.multiple_of(owner * width, width), width)]

    half = depth // 2

    def w_copy(step, way):
        back = 2 * (step - 1)
        owner = lax.rem(dp + (nd - back if way == 0 else back), nd)
        if step < steps:
            lo, rows = 0, depth
        else:
            lo, rows = (0, half) if way == 0 else (half, half)
        dst = w_at(owner, lo, rows)
        src = w_hbm.at[pl.ds(lo, rows), :] if step == 1 else dst
        return pltpu.make_async_remote_copy(
            src_ref=src, dst_ref=dst,
            send_sem=wsend.at[step - 1, way], recv_sem=wrecv.at[step - 1, way],
            device_id={"dp": right if way == 0 else left}, device_id_type=MESH,
        )

    def w_arrived(step, way):
        ahead = 2 * step
        owner = lax.rem(dp + (nd - ahead if way == 0 else ahead), nd)
        if step < steps:
            lo, rows = 0, depth
        else:
            lo, rows = (0, half) if way == 0 else (half, half)
        dst = w_at(owner, lo, rows)
        pltpu.make_async_remote_copy(
            src_ref=dst, dst_ref=dst,
            send_sem=wsend.at[step - 1, way], recv_sem=wrecv.at[step - 1, way],
            device_id={"dp": right}, device_id_type=MESH,
        ).wait_recv()

    def p_copy(step, way):
        ahead = 2 * step
        owner = lax.rem(dp + (nd - ahead if way == 0 else ahead), nd)
        dst = w_at(owner)
        return pltpu.make_async_remote_copy(
            src_ref=w_hbm if step == 0 else dst, dst_ref=dst,
            send_sem=psend.at[step, way], recv_sem=precv.at[step, way],
            device_id={"dp": partner}, device_id_type=MESH,
        )

    def p_arrived(step, way):
        ahead = 2 * step
        owner = lax.rem(partner + (nd - ahead if way == 0 else ahead), nd)
        dst = w_at(owner)
        pltpu.make_async_remote_copy(
            src_ref=dst, dst_ref=dst,
            send_sem=psend.at[step, way], recv_sem=precv.at[step, way],
            device_id={"dp": partner}, device_id_type=MESH,
        ).wait_recv()

    p_list = [(0, 0)] + [(s, w) for s in range(1, steps) for w in (0, 1)] + [(steps, 0)]

    def w_step(step):
        for way in (0, 1):
            w_arrived(step, way)
        if step < steps:
            for way in (0, 1):
                w_copy(step + 1, way).start()
                p_copy(step, way).start()
        else:
            p_copy(step, 0).start()

    for which in range(3):
        own(which).start()
    own_w = pltpu.make_async_copy(w_hbm, w_at(dp), loc_sem.at[3])
    own_w.start()
    barrier()
    start_all(0)
    for way in (0, 1):
        w_copy(1, way).start()
    p_copy(0, 0).start()
    start_all(1)

    for row, ref in ((0, qg_ref), (1, kg_ref)):
        g = ref[...]
        gains[row : row + 1, :] = jnp.concatenate([g, g], axis=1)
    lane = lax.broadcasted_iota(jnp.int32, (1, lanes), 1)
    low_half = lax.rem(lane, head) < head // 2
    first_map = lane < head
    ri = lax.broadcasted_iota(jnp.int32, (lanes, lanes), 0) // head
    ci = lax.broadcasted_iota(jnp.int32, (lanes, lanes), 1) // head
    ones = (ri == ci).astype(jnp.float32).astype(jnp.bfloat16)
    acc[...] = jnp.zeros_like(acc)

    def rotate(raw, number, gain):
        x = raw.astype(jnp.float32)
        sq = x * x
        hi = sq.astype(jnp.bfloat16)
        lo = (sq - hi.astype(jnp.float32)).astype(jnp.bfloat16)
        total = jnp.dot(hi, ones, preferred_element_type=jnp.float32) + jnp.dot(
            lo, ones, preferred_element_type=jnp.float32
        )
        y = x * lax.rsqrt(total * (1.0 / head) + EPSILON) * gain
        cb, sb = base_ref[0, pl.ds(number, 1), :], base_ref[1, pl.ds(number, 1), :]
        co, so = offs_ref[0], offs_ref[1]
        cosine = cb * co - sb * so
        sine = sb * co + cb * so
        other = jnp.where(
            low_half, pltpu.roll(y, lanes - head // 2, 1), pltpu.roll(y, head // 2, 1)
        )
        return (y * cosine + other * sine).astype(jnp.bfloat16)

    own(0).wait()

    def key_block(t, c):
        @pl.when(t > 0)
        def _():
            chunk_arrived(0, t)

        number = peer_of(t)
        krot[pl.ds(pl.multiple_of(number * tok, tok), tok), :] = rotate(
            kraw[number], number, gains[1:2, :]
        )
        return c

    lax.fori_loop(0, n, key_block, 0)
    start_far(2)
    w_step(1)

    own(1).wait()
    own(2).wait()
    own_w.wait()

    def value_block(t, c):
        chunk_arrived(1, t)
        return c

    mid = (3 * n) // 4
    lax.fori_loop(1, mid, value_block, 0)
    if steps >= 2:
        w_step(2)
    lax.fori_loop(mid, n, value_block, 0)
    for s in range(3, steps + 1):
        w_step(s)

    lam = lam_ref[me]
    span = CHUNK * tok

    def attend(number):
        q = rotate(qraw[number], number, gains[0:1, :]) * jnp.bfloat16(head**-0.5)
        zero = jnp.zeros_like(q)
        both = jnp.concatenate(
            [jnp.where(first_map, q, zero), jnp.where(first_map, zero, q)], axis=0
        )
        full = number // CHUNK

        def score(j):
            keys = krot[pl.ds(pl.multiple_of(j * span, span), span), :]
            return lax.dot_general(
                both, keys, (((1,), (1,)), ((), ())), preferred_element_type=jnp.float32
            )

        def highest(s, m):
            for c in range(CHUNK):
                m = jnp.maximum(m, s[:, c * tok : (c + 1) * tok])
            return m

        def body(j, m):
            s = score(j)
            sc[j] = s
            return highest(s, m)

        m = lax.fori_loop(0, full, body, jnp.full((2 * tok, tok), NEG, jnp.float32))
        s = score(full)
        row = lax.rem(lax.broadcasted_iota(jnp.int32, s.shape, 0), tok) + number * tok
        col = lax.broadcasted_iota(jnp.int32, s.shape, 1) + full * span
        s = jnp.where(col <= row, s, NEG)
        sc[full] = s
        m = jnp.max(highest(s, m), axis=-1, keepdims=True)

        def expo(j, total):
            e = jnp.exp2((sc[j] - m) * LOG2E)
            sc[j] = e
            for c in range(CHUNK):
                total = total + e[:, c * tok : (c + 1) * tok]
            return total

        total = lax.fori_loop(0, full + 1, expo, jnp.zeros((2 * tok, tok), jnp.float32))
        total = 1.0 / jnp.sum(total, axis=-1, keepdims=True)
        one, two = total[:tok], total[tok:] * lam

        def mix(j, o):
            p = (sc[j, :tok, :] * one - sc[j, tok:, :] * two).astype(jnp.bfloat16)
            return o + jnp.dot(
                p, vall[pl.ds(pl.multiple_of(j * span, span), span), :],
                preferred_element_type=jnp.float32,
            )

        o = lax.fori_loop(0, full + 1, mix, jnp.zeros((tok, vall.shape[1]), jnp.float32))
        o = o * lax.rsqrt(jnp.mean(o * o, axis=-1, keepdims=True) + EPSILON)
        return (o * hg_ref[...] * OUT_SCALE).astype(jnp.bfloat16)

    def query_block(s, c):
        t = n - 1 - s
        number = peer_of(t)

        @pl.when(t > 0)
        def _():
            chunk_arrived(2, t)

        osend[number] = attend(number)

        @pl.when(t > 0)
        def _():
            chunk_copy(3, t).start()

        return c

    lax.fori_loop(0, n, query_block, 0)

    for step, way in p_list:
        p_arrived(step, way)

    def project(block, src):
        rows = pl.ds(pl.multiple_of(block * tok, tok), tok)
        acc[...] += jnp.dot(src, w_all[rows, :], preferred_element_type=jnp.float32)

    project(me, osend[me])

    def head_block(s, c):
        t = n - s
        chunk_arrived(3, t)
        block = peer_of(t)
        project(block, oin[block])
        return c

    lax.fori_loop(1, n, head_block, 0)
    out_ref[0] = acc[...].astype(jnp.bfloat16)

    def sent(t, c):
        for which in range(4):
            chunk_copy(which, t).wait_send()
        return c

    lax.fori_loop(1, n, sent, 0)
    for step in range(1, steps + 1):
        for way in (0, 1):
            w_copy(step, way).wait_send()
    for step, way in p_list:
        p_copy(step, way).wait_send()


def local(query_rows, key_rows, value_rows, query_gain, key_gain, lambdas, head_gain, out_weight):
    n, nd = lax.axis_size("sp"), lax.axis_size("dp")
    head, vdim = query_gain.shape[0], head_gain.shape[0]
    _, tok, total = query_rows.shape
    lanes = 2 * head
    assert lambdas.shape[0] == n and total == n * lanes and vdim == lanes and tok == vdim
    base, offs = rope_tables(n, tok, head)
    columns = out_weight.shape[1] * nd
    steps = nd // 4
    anywhere = pl.BlockSpec(memory_space=pl.ANY)
    vmem = pl.BlockSpec(memory_space=pltpu.VMEM)
    smem = pl.BlockSpec(memory_space=pltpu.SMEM)
    dma = pltpu.SemaphoreType.DMA
    bf16, f32 = jnp.bfloat16, jnp.float32
    return pl.pallas_call(
        functools.partial(kernel, n, nd, head),
        out_shape=jax.ShapeDtypeStruct((1, tok, columns), bf16),
        in_specs=[anywhere] * 4 + [vmem, vmem, smem, vmem, vmem, vmem],
        out_specs=vmem,
        scratch_shapes=[
            pltpu.VMEM((n, tok, lanes), bf16),
            pltpu.VMEM((n, tok, lanes), bf16),
            pltpu.VMEM((n * tok, lanes), bf16),
            pltpu.VMEM((n * tok, vdim), bf16),
            pltpu.VMEM((n, tok, vdim), bf16),
            pltpu.VMEM((n, tok, vdim), bf16),
            pltpu.VMEM((n * vdim, columns), bf16),
            pltpu.VMEM((n // CHUNK, 2 * tok, CHUNK * tok), f32),
            pltpu.VMEM((tok, columns), f32),
            pltpu.VMEM((8, lanes), f32),
            dma((4,)), dma((4, n)), dma((4, n)),
            dma((steps, 2)), dma((steps, 2)), dma((steps + 1, 2)), dma((steps + 1, 2)),
        ],
        compiler_params=pltpu.CompilerParams(
            collective_id=0, has_side_effects=True, vmem_limit_bytes=40 * 2**20
        ),
    )(
        query_rows, key_rows, value_rows, out_weight,
        query_gain.reshape(1, head), key_gain.reshape(1, head), lambdas,
        head_gain.reshape(1, vdim), jnp.asarray(base), jnp.asarray(offs),
    )


def solution(mesh):
    placed = (
        P(("grp", "dp"), "sp", None),
        P(("grp", "dp"), "sp", None),
        P(("grp", "dp"), "sp", None),
        P(),
        P(),
        P(),
        P(),
        P(None, "dp"),
    )
    return jax.shard_map(
        local, mesh=mesh, in_specs=placed, out_specs=P(("grp", "dp"), "sp", None), check_vma=False
    )
```

```python
import functools

import jax
import jax.numpy as jnp
import numpy as np
from jax import lax
from jax.experimental import pallas as pl
from jax.experimental.pallas import tpu as pltpu
from jax.sharding import PartitionSpec as P

EPSILON = 1e-06
OUT_SCALE = 0.8
LOG2E = 1.4426950408889634
NEG = -1e30
MESH = pl.DeviceIdType.MESH
CHUNK = 4


def rope_tables(blocks, block, head):
    half = head // 2
    lane = np.arange(2 * head) % head
    inverse = 10000.0 ** (-(lane % half).astype(np.float64) / half)
    sign = np.where(lane < half, -1.0, 1.0)

    def pair(positions):
        angle = positions[:, None] * inverse[None, :]
        return np.stack([np.cos(angle), sign * np.sin(angle)]).astype(np.float32)

    return np.concatenate(
        [pair(np.arange(blocks) * float(block)), pair(np.arange(block).astype(np.float64))], axis=1
    )


def kernel(
    n, nd, head,
    q_hbm, k_hbm, v_hbm, w_hbm, qg_ref, kg_ref, lam_ref, hg_ref, table_ref,
    out_ref,
    kraw, vraw, qraw, krot, vall, osend, oin, w_all, sc, acc, gains,
    loc_sem, send_sem, recv_sem, wsend, wrecv, psend, precv, ready, lead_in,
):
    me = lax.axis_index("sp")
    dp = lax.axis_index("dp")
    lead_ring = (dp == 0) & (lax.axis_index("grp") == 0)
    lead_plane = (me == 0) & (lax.axis_index("grp") == 0)
    is_lead = lead_ring & lead_plane
    core = lax.rem(dp, 2)
    partner = dp + 1 - 2 * core
    reach = max(nd // 8, 1)
    along = [
        (k, way, lax.rem(dp + (2 * k if way == 0 else nd - 2 * k), nd))
        for k in range(1, reach + 1)
        for way in (0, 1)
    ]
    beside = [d for _, _, d in along] + [partner]
    tok = out_ref.shape[1]
    depth, width = w_hbm.shape
    lanes = 2 * head

    first = jnp.where(lead_ring, 1, 0)
    pos = lax.rem(me - first + n, n)

    def at(p):
        return lax.rem(p + first, n)

    def leads(d):
        return lead_plane & (d == 0)

    beside_lead = sum(leads(d).astype(jnp.int32) for d in beside)

    def enter():
        sem = pltpu.get_barrier_semaphore()

        @pl.when(jnp.logical_not(is_lead))
        def _():
            for d in beside:
                pl.semaphore_signal(sem, inc=1, device_id={"dp": d}, device_id_type=MESH)

        pl.semaphore_wait(sem, len(beside) - beside_lead + jnp.where(pos > 0, 1, 0))

        @pl.when(pos < n - 1)
        def _():
            pl.semaphore_signal(sem, inc=1, device_id={"sp": at(pos + 1)}, device_id_type=MESH)

        @pl.when(is_lead)
        def _():
            for d in beside:
                pl.semaphore_signal(lead_in, inc=1, device_id={"dp": d}, device_id_type=MESH)

        def tell(p, c):
            pl.semaphore_signal(ready.at[me], inc=1, device_id={"sp": at(p)}, device_id_type=MESH)
            return c

        lax.fori_loop(0, pos, tell, 0)

    raws = (kraw, vraw, qraw)

    def chunk_copy(which, peer):
        if which == 3:
            src = osend.at[peer]
            dst = oin.at[:, pl.ds(pl.multiple_of(me * tok, tok), tok)]
        else:
            src = (k_hbm, v_hbm, q_hbm)[which].at[
                0, :, pl.ds(pl.multiple_of(peer * lanes, lanes), lanes)
            ]
            dst = raws[which].at[me]
        return pltpu.make_async_remote_copy(
            src_ref=src, dst_ref=dst,
            send_sem=send_sem.at[which, peer], recv_sem=recv_sem.at[which, me],
            device_id={"sp": peer}, device_id_type=MESH,
        )

    def chunk_arrived(which, peer):
        if which == 3:
            dst = oin.at[:, pl.ds(pl.multiple_of(peer * tok, tok), tok)]
        else:
            dst = raws[which].at[peer]
        pltpu.make_async_remote_copy(
            src_ref=dst, dst_ref=dst,
            send_sem=send_sem.at[which, peer], recv_sem=recv_sem.at[which, peer],
            device_id={"sp": peer}, device_id_type=MESH,
        ).wait_recv()

    def own(which):
        cols = pl.ds(pl.multiple_of(me * lanes, lanes), lanes)
        return pltpu.make_async_copy(
            (k_hbm, v_hbm, q_hbm)[which].at[0, :, cols], raws[which].at[me], loc_sem.at[which]
        )

    def w_at(owner, lo=0, rows=None):
        rows = depth if rows is None else rows
        return w_all.at[pl.ds(lo, rows), pl.ds(pl.multiple_of(owner * width, width), width)]

    half = depth // 2

    def away(device, chips, way):
        return lax.rem(device + (nd - 2 * chips if way == 0 else 2 * chips), nd)

    def remote(src, dst, send, recv, d):
        return pltpu.make_async_remote_copy(
            src_ref=src, dst_ref=dst, send_sem=send, recv_sem=recv,
            device_id={"dp": d}, device_id_type=MESH,
        )

    def w_part(phase, k, way):
        if phase == 0 or k < reach:
            return 0, depth
        return (0, half) if way == 0 else (half, half)

    def w_copy(phase, k, way, d):
        dst = w_at(away(dp, phase * k, way), *w_part(phase, k, way))
        i = phase * reach + k - 1
        return remote(w_hbm if phase == 0 else dst, dst, wsend.at[i, way], wrecv.at[i, way], d)

    def w_arrived(phase, k, way):
        dst = w_at(away(dp, k + phase * reach, way), *w_part(phase, k, way))
        i = phase * reach + k - 1
        remote(dst, dst, wsend.at[i, way], wrecv.at[i, way], partner).wait_recv()

    p_list = [(0, 0)] + [(c, way) for c in range(1, 2 * reach) for way in (0, 1)] + [(2 * reach, 0)]

    def p_copy(chips, way):
        dst = w_at(away(dp, chips, way))
        return remote(
            w_hbm if chips == 0 else dst, dst, psend.at[chips, way], precv.at[chips, way], partner
        )

    def p_arrived(chips, way):
        dst = w_at(away(partner, chips, way))
        remote(dst, dst, psend.at[chips, way], precv.at[chips, way], partner).wait_recv()

    def w_first(to_lead):
        copies = [(w_copy(0, k, way, d), d) for k, way, d in along] + [(p_copy(0, 0), partner)]
        for copy, d in copies:

            @pl.when(leads(d) if to_lead else jnp.logical_not(leads(d)))
            def _():
                copy.start()

    far = [d for k, _, d in along if k == reach]

    def w_on():
        for k in range(1, reach + 1):
            for way in (0, 1):
                w_arrived(0, k, way)
                w_copy(1, k, way, far[way]).start()
                p_copy(k, way).start()

    def w_rest():
        for k in range(1, reach + 1):
            for way in (0, 1):
                w_arrived(1, k, way)
                if k < reach:
                    p_copy(reach + k, way).start()
        p_copy(2 * reach, 0).start()

    for which in range(3):
        own(which).start()
    own_w = pltpu.make_async_copy(w_hbm, w_at(dp), loc_sem.at[3])
    own_w.start()
    enter()

    def send_to(p):
        for which in range(3):
            chunk_copy(which, at(p)).start()

    def send_lower(s, c):
        send_to(pos - 1 - s)
        return c

    def send_upper(p, c):
        pl.semaphore_wait(ready.at[at(p)], 1)
        send_to(p)
        return c

    w_first(False)
    lax.fori_loop(0, pos, send_lower, 0)
    lax.fori_loop(pos + 1, n, send_upper, 0)

    @pl.when(jnp.logical_not(is_lead) & (beside_lead > 0))
    def _():
        pl.semaphore_wait(lead_in, beside_lead)
        w_first(True)


    for row, ref in ((0, qg_ref), (1, kg_ref)):
        g = ref[...]
        gains[row : row + 1, :] = jnp.concatenate([g, g], axis=1)
    lane = lax.broadcasted_iota(jnp.int32, (1, lanes), 1)
    low_half = lax.rem(lane, head) < head // 2
    first_map = lane < head
    ri = lax.broadcasted_iota(jnp.int32, (lanes, lanes), 0) // head
    ci = lax.broadcasted_iota(jnp.int32, (lanes, lanes), 1) // head
    ones = (ri == ci).astype(jnp.float32).astype(jnp.bfloat16)
    krot[...] = jnp.zeros_like(krot)
    vall[...] = jnp.zeros_like(vall)

    def rotate(raw, number, gain):
        x = raw.astype(jnp.float32)
        sq = x * x
        hi = sq.astype(jnp.bfloat16)
        lo = (sq - hi.astype(jnp.float32)).astype(jnp.bfloat16)
        total = jnp.dot(hi, ones, preferred_element_type=jnp.float32) + jnp.dot(
            lo, ones, preferred_element_type=jnp.float32
        )
        y = x * lax.rsqrt(total * (1.0 / head) + EPSILON) * gain
        cb, sb = table_ref[0, pl.ds(number, 1), :], table_ref[1, pl.ds(number, 1), :]
        co, so = table_ref[0, n : n + tok, :], table_ref[1, n : n + tok, :]
        cosine = cb * co - sb * so
        sine = sb * co + cb * so
        other = jnp.where(
            low_half, pltpu.roll(y, lanes - head // 2, 1), pltpu.roll(y, head // 2, 1)
        )
        return (y * cosine + other * sine).astype(jnp.bfloat16)

    lam = lam_ref[me]
    span = CHUNK * tok

    def attend(number):
        q = rotate(qraw[number], number, gains[0:1, :]) * jnp.bfloat16(head**-0.5)
        zero = jnp.zeros_like(q)
        both = jnp.concatenate(
            [jnp.where(first_map, q, zero), jnp.where(first_map, zero, q)], axis=0
        )
        full = number // CHUNK

        def score(j):
            keys = krot[pl.ds(pl.multiple_of(j * span, span), span), :]
            return lax.dot_general(
                both, keys, (((1,), (1,)), ((), ())), preferred_element_type=jnp.float32
            )

        def highest(s, m):
            for c in range(CHUNK):
                m = jnp.maximum(m, s[:, c * tok : (c + 1) * tok])
            return m

        def body(j, m):
            s = score(j)
            sc[j] = s
            return highest(s, m)

        m = lax.fori_loop(0, full, body, jnp.full((2 * tok, tok), NEG, jnp.float32))
        s = score(full)
        row = lax.rem(lax.broadcasted_iota(jnp.int32, s.shape, 0), tok) + number * tok
        col = lax.broadcasted_iota(jnp.int32, s.shape, 1) + full * span
        s = jnp.where(col <= row, s, NEG)
        sc[full] = s
        m = jnp.max(highest(s, m), axis=-1, keepdims=True)

        def expo(j, total):
            e = jnp.exp2((sc[j] - m) * LOG2E)
            sc[j] = e
            for c in range(CHUNK):
                total = total + e[:, c * tok : (c + 1) * tok]
            return total

        total = lax.fori_loop(0, full + 1, expo, jnp.zeros((2 * tok, tok), jnp.float32))
        total = 1.0 / jnp.sum(total, axis=-1, keepdims=True)
        one, two = total[:tok], total[tok:] * lam

        def mix(j, o):
            p = (sc[j, :tok, :] * one - sc[j, tok:, :] * two).astype(jnp.bfloat16)
            return o + jnp.dot(
                p, vall[pl.ds(pl.multiple_of(j * span, span), span), :],
                preferred_element_type=jnp.float32,
            )

        o = lax.fori_loop(0, full + 1, mix, jnp.zeros((tok, vall.shape[1]), jnp.float32))
        o = o * lax.rsqrt(jnp.mean(o * o, axis=-1, keepdims=True) + EPSILON)
        return (o * hg_ref[...] * OUT_SCALE).astype(jnp.bfloat16)

    for which in range(3):
        own(which).wait()

    w_on_turn = jnp.where(is_lead, n // 16, (3 * n) // 8)
    w_rest_turn = jnp.where(is_lead, n // 2, jnp.where(me < n // 2, (3 * n) // 4, n - 1))

    def turn(s, c):
        @pl.when(s == w_on_turn)
        def _():
            w_on()

        @pl.when(s == w_rest_turn)
        def _():
            w_rest()

        number = s

        @pl.when(number != me)
        def _():
            for which in range(3):
                chunk_arrived(which, number)

        rows = pl.ds(pl.multiple_of(number * tok, tok), tok)
        krot[rows, :] = rotate(kraw[number], number, gains[1:2, :])
        vall[rows, :] = vraw[number]

        o = attend(number)

        @pl.when(number == me)
        def _():
            oin[:, pl.ds(pl.multiple_of(me * tok, tok), tok)] = o

        @pl.when(number != me)
        def _():
            osend[number] = o
            chunk_copy(3, number).start()

        return c

    lax.fori_loop(0, n, turn, 0)
    own_w.wait()
    for chips, way in p_list:
        p_arrived(chips, way)

    acc[...] = jnp.zeros_like(acc)
    groups = n // CHUNK

    def head_group(turn, c):
        g = lax.rem(turn + first, groups)
        for j in range(CHUNK):
            block = g * CHUNK + j

            @pl.when(block != me)
            def _():
                chunk_arrived(3, block)

        cols = pl.ds(pl.multiple_of(g * span, span), span)
        acc[...] += jnp.dot(oin[:, cols], w_all[cols, :], preferred_element_type=jnp.float32)
        return c

    lax.fori_loop(0, groups, head_group, 0)
    out_ref[0] = acc[...].astype(jnp.bfloat16)

    def sent(p, c):
        @pl.when(p != me)
        def _():
            for which in range(4):
                chunk_copy(which, p).wait_send()

        return c

    lax.fori_loop(0, n, sent, 0)
    for phase in (0, 1):
        for k, way, d in along:
            w_copy(phase, k, way, d).wait_send()
    for chips, way in p_list:
        p_copy(chips, way).wait_send()


def local(query_rows, key_rows, value_rows, query_gain, key_gain, lambdas, head_gain, out_weight):
    n, nd = lax.axis_size("sp"), lax.axis_size("dp")
    head, vdim = query_gain.shape[0], head_gain.shape[0]
    _, tok, total = query_rows.shape
    lanes = 2 * head
    assert lambdas.shape[0] == n and total == n * lanes and vdim == lanes and tok == vdim
    table = rope_tables(n, tok, head)
    columns = out_weight.shape[1] * nd
    reach = max(nd // 8, 1)
    anywhere = pl.BlockSpec(memory_space=pl.ANY)
    vmem = pl.BlockSpec(memory_space=pltpu.VMEM)
    smem = pl.BlockSpec(memory_space=pltpu.SMEM)
    dma = pltpu.SemaphoreType.DMA
    bf16, f32 = jnp.bfloat16, jnp.float32
    return pl.pallas_call(
        functools.partial(kernel, n, nd, head),
        out_shape=jax.ShapeDtypeStruct((1, tok, columns), bf16),
        in_specs=[anywhere] * 4 + [vmem, vmem, smem, vmem, vmem],
        out_specs=vmem,
        scratch_shapes=[
            pltpu.VMEM((n, tok, lanes), bf16),
            pltpu.VMEM((n, tok, vdim), bf16),
            pltpu.VMEM((n, tok, lanes), bf16),
            pltpu.VMEM((n * tok, lanes), bf16),
            pltpu.VMEM((n * tok, vdim), bf16),
            pltpu.VMEM((n, tok, vdim), bf16),
            pltpu.VMEM((tok, n * vdim), bf16),
            pltpu.VMEM((n * vdim, columns), bf16),
            pltpu.VMEM((n // CHUNK, 2 * tok, CHUNK * tok), f32),
            pltpu.VMEM((tok, columns), f32),
            pltpu.VMEM((8, lanes), f32),
            dma((4,)), dma((4, n)), dma((4, n)),
            dma((2 * reach, 2)), dma((2 * reach, 2)),
            dma((2 * reach + 1, 2)), dma((2 * reach + 1, 2)),
            pltpu.SemaphoreType.REGULAR((n,)), pltpu.SemaphoreType.REGULAR,
        ],
        compiler_params=pltpu.CompilerParams(
            collective_id=0, has_side_effects=True, vmem_limit_bytes=67_043_328
        ),
    )(
        query_rows, key_rows, value_rows, out_weight,
        query_gain.reshape(1, head), key_gain.reshape(1, head), lambdas,
        head_gain.reshape(1, vdim), jnp.asarray(table),
    )


def solution(mesh):
    placed = (
        P(("grp", "dp"), "sp", None),
        P(("grp", "dp"), "sp", None),
        P(("grp", "dp"), "sp", None),
        P(),
        P(),
        P(),
        P(),
        P(None, "dp"),
    )
    return jax.shard_map(
        local, mesh=mesh, in_specs=placed, out_specs=P(("grp", "dp"), "sp", None), check_vma=False
    )
```

```python
import functools

import jax
import jax.numpy as jnp
import numpy as np
from jax import lax
from jax.experimental import pallas as pl
from jax.experimental.pallas import tpu as pltpu
from jax.sharding import PartitionSpec as P

EPSILON = 1e-06
OUT_SCALE = 0.8
LOG2E = 1.4426950408889634
NEG = -1e30
MESH = pl.DeviceIdType.MESH
CHUNK = 4


def rope_tables(blocks, block, head):
    half = head // 2
    lane = np.arange(2 * head) % head
    inverse = 10000.0 ** (-(lane % half).astype(np.float64) / half)
    sign = np.where(lane < half, -1.0, 1.0)

    def pair(positions):
        angle = positions[:, None] * inverse[None, :]
        return np.stack([np.cos(angle), sign * np.sin(angle)]).astype(np.float32)

    return np.concatenate(
        [pair(np.arange(blocks) * float(block)), pair(np.arange(block).astype(np.float64))], axis=1
    )


def kernel(
    n, nd, head,
    q_hbm, k_hbm, v_hbm, w_hbm, qg_ref, kg_ref, lam_ref, hg_ref, table_ref,
    out_ref,
    kraw, vraw, qraw, krot, vall, osend, oin, w_all, sc, acc, gains,
    loc_sem, send_sem, recv_sem, wsend, wrecv, psend, precv, ready, lead_in,
):
    me = lax.axis_index("sp")
    dp = lax.axis_index("dp")
    lead_ring = (dp == 0) & (lax.axis_index("grp") == 0)
    lead_plane = (me == 0) & (lax.axis_index("grp") == 0)
    is_lead = lead_ring & lead_plane
    core = lax.rem(dp, 2)
    partner = dp + 1 - 2 * core
    reach = max(nd // 8, 1)
    along = [
        (k, way, lax.rem(dp + (2 * k if way == 0 else nd - 2 * k), nd))
        for k in range(1, reach + 1)
        for way in (0, 1)
    ]
    beside = [d for _, _, d in along] + [partner]
    tok = out_ref.shape[1]
    depth, width = w_hbm.shape
    lanes = 2 * head

    first = jnp.where(lead_ring, 1, 0)
    pos = lax.rem(me - first + n, n)

    def at(p):
        return lax.rem(p + first, n)

    def leads(d):
        return lead_plane & (d == 0)

    beside_lead = sum(leads(d).astype(jnp.int32) for d in beside)

    def enter():
        sem = pltpu.get_barrier_semaphore()

        @pl.when(jnp.logical_not(is_lead))
        def _():
            for d in beside:
                pl.semaphore_signal(sem, inc=1, device_id={"dp": d}, device_id_type=MESH)

        pl.semaphore_wait(sem, len(beside) - beside_lead + jnp.where(pos > 0, 1, 0))

        @pl.when(pos < n - 1)
        def _():
            pl.semaphore_signal(sem, inc=1, device_id={"sp": at(pos + 1)}, device_id_type=MESH)

        @pl.when(is_lead)
        def _():
            for d in beside:
                pl.semaphore_signal(lead_in, inc=1, device_id={"dp": d}, device_id_type=MESH)

        def tell(p, c):
            pl.semaphore_signal(ready.at[me], inc=1, device_id={"sp": at(p)}, device_id_type=MESH)
            return c

        lax.fori_loop(0, pos, tell, 0)

    raws = (kraw, vraw, qraw)

    def chunk_copy(which, peer):
        if which == 3:
            src = osend.at[peer]
            dst = oin.at[:, pl.ds(pl.multiple_of(me * tok, tok), tok)]
        else:
            src = (k_hbm, v_hbm, q_hbm)[which].at[
                0, :, pl.ds(pl.multiple_of(peer * lanes, lanes), lanes)
            ]
            dst = raws[which].at[me]
        return pltpu.make_async_remote_copy(
            src_ref=src, dst_ref=dst,
            send_sem=send_sem.at[which, peer], recv_sem=recv_sem.at[which, me],
            device_id={"sp": peer}, device_id_type=MESH,
        )

    def chunk_arrived(which, peer):
        if which == 3:
            dst = oin.at[:, pl.ds(pl.multiple_of(peer * tok, tok), tok)]
        else:
            dst = raws[which].at[peer]
        pltpu.make_async_remote_copy(
            src_ref=dst, dst_ref=dst,
            send_sem=send_sem.at[which, peer], recv_sem=recv_sem.at[which, peer],
            device_id={"sp": peer}, device_id_type=MESH,
        ).wait_recv()

    def own(which):
        cols = pl.ds(pl.multiple_of(me * lanes, lanes), lanes)
        return pltpu.make_async_copy(
            (k_hbm, v_hbm, q_hbm)[which].at[0, :, cols], raws[which].at[me], loc_sem.at[which]
        )

    def w_at(owner, lo=0, rows=None):
        rows = depth if rows is None else rows
        return w_all.at[pl.ds(lo, rows), pl.ds(pl.multiple_of(owner * width, width), width)]

    half = depth // 2

    def away(device, chips, way):
        return lax.rem(device + (nd - 2 * chips if way == 0 else 2 * chips), nd)

    def remote(src, dst, send, recv, d):
        return pltpu.make_async_remote_copy(
            src_ref=src, dst_ref=dst, send_sem=send, recv_sem=recv,
            device_id={"dp": d}, device_id_type=MESH,
        )

    def w_part(phase, k, way):
        if phase == 0 or k < reach:
            return 0, depth
        return (0, half) if way == 0 else (half, half)

    def w_copy(phase, k, way, d):
        dst = w_at(away(dp, phase * k, way), *w_part(phase, k, way))
        i = phase * reach + k - 1
        return remote(w_hbm if phase == 0 else dst, dst, wsend.at[i, way], wrecv.at[i, way], d)

    def w_arrived(phase, k, way):
        dst = w_at(away(dp, k + phase * reach, way), *w_part(phase, k, way))
        i = phase * reach + k - 1
        remote(dst, dst, wsend.at[i, way], wrecv.at[i, way], partner).wait_recv()

    p_list = [(0, 0)] + [(c, way) for c in range(1, 2 * reach) for way in (0, 1)] + [(2 * reach, 0)]

    def p_copy(chips, way):
        dst = w_at(away(dp, chips, way))
        return remote(
            w_hbm if chips == 0 else dst, dst, psend.at[chips, way], precv.at[chips, way], partner
        )

    def p_arrived(chips, way):
        dst = w_at(away(partner, chips, way))
        remote(dst, dst, psend.at[chips, way], precv.at[chips, way], partner).wait_recv()

    def w_first(to_lead):
        copies = [(w_copy(0, k, way, d), d) for k, way, d in along] + [(p_copy(0, 0), partner)]
        for copy, d in copies:

            @pl.when(leads(d) if to_lead else jnp.logical_not(leads(d)))
            def _():
                copy.start()

    far = [d for k, _, d in along if k == reach]

    def w_on():
        for k in range(1, reach + 1):
            for way in (0, 1):
                w_arrived(0, k, way)
                w_copy(1, k, way, far[way]).start()
                p_copy(k, way).start()

    def w_rest():
        for k in range(1, reach + 1):
            for way in (0, 1):
                w_arrived(1, k, way)
                if k < reach:
                    p_copy(reach + k, way).start()
        p_copy(2 * reach, 0).start()

    for which in range(3):
        own(which).start()
    own_w = pltpu.make_async_copy(w_hbm, w_at(dp), loc_sem.at[3])
    own_w.start()
    enter()

    def send_to(p):
        for which in range(3):
            chunk_copy(which, at(p)).start()

    def send_lower(s, c):
        k = s // 2
        both_ways = jnp.where(lax.rem(s, 2) == 0, pos - 1 - k, k)
        send_to(jnp.where(pos > n // 2, both_ways, pos - 1 - s))
        return c

    def send_upper(p, c):
        pl.semaphore_wait(ready.at[at(p)], 1)
        send_to(p)
        return c

    w_first(False)
    lax.fori_loop(0, pos, send_lower, 0)
    lax.fori_loop(pos + 1, n, send_upper, 0)

    @pl.when(jnp.logical_not(is_lead) & (beside_lead > 0))
    def _():
        pl.semaphore_wait(lead_in, beside_lead)
        w_first(True)


    for row, ref in ((0, qg_ref), (1, kg_ref)):
        g = ref[...]
        gains[row : row + 1, :] = jnp.concatenate([g, g], axis=1)
    lane = lax.broadcasted_iota(jnp.int32, (1, lanes), 1)
    low_half = lax.rem(lane, head) < head // 2
    first_map = lane < head
    ri = lax.broadcasted_iota(jnp.int32, (lanes, lanes), 0) // head
    ci = lax.broadcasted_iota(jnp.int32, (lanes, lanes), 1) // head
    ones = (ri == ci).astype(jnp.float32).astype(jnp.bfloat16)
    krot[...] = jnp.zeros_like(krot)
    vall[...] = jnp.zeros_like(vall)

    def rotate(raw, number, gain):
        x = raw.astype(jnp.float32)
        sq = x * x
        hi = sq.astype(jnp.bfloat16)
        lo = (sq - hi.astype(jnp.float32)).astype(jnp.bfloat16)
        total = jnp.dot(hi, ones, preferred_element_type=jnp.float32) + jnp.dot(
            lo, ones, preferred_element_type=jnp.float32
        )
        y = x * lax.rsqrt(total * (1.0 / head) + EPSILON) * gain
        cb, sb = table_ref[0, pl.ds(number, 1), :], table_ref[1, pl.ds(number, 1), :]
        co, so = table_ref[0, n : n + tok, :], table_ref[1, n : n + tok, :]
        cosine = cb * co - sb * so
        sine = sb * co + cb * so
        other = jnp.where(
            low_half, pltpu.roll(y, lanes - head // 2, 1), pltpu.roll(y, head // 2, 1)
        )
        return (y * cosine + other * sine).astype(jnp.bfloat16)

    lam = lam_ref[me]
    span = CHUNK * tok

    def attend(number):
        q = rotate(qraw[number], number, gains[0:1, :]) * jnp.bfloat16(head**-0.5)
        zero = jnp.zeros_like(q)
        both = jnp.concatenate(
            [jnp.where(first_map, q, zero), jnp.where(first_map, zero, q)], axis=0
        )
        full = number // CHUNK

        def score(j):
            keys = krot[pl.ds(pl.multiple_of(j * span, span), span), :]
            return lax.dot_general(
                both, keys, (((1,), (1,)), ((), ())), preferred_element_type=jnp.float32
            )

        def highest(s, m):
            for c in range(CHUNK):
                m = jnp.maximum(m, s[:, c * tok : (c + 1) * tok])
            return m

        def body(j, m):
            s = score(j)
            sc[j] = s
            return highest(s, m)

        m = lax.fori_loop(0, full, body, jnp.full((2 * tok, tok), NEG, jnp.float32))
        s = score(full)
        row = lax.rem(lax.broadcasted_iota(jnp.int32, s.shape, 0), tok) + number * tok
        col = lax.broadcasted_iota(jnp.int32, s.shape, 1) + full * span
        s = jnp.where(col <= row, s, NEG)
        sc[full] = s
        m = jnp.max(highest(s, m), axis=-1, keepdims=True)

        def expo(j, total):
            e = jnp.exp2((sc[j] - m) * LOG2E)
            sc[j] = e
            for c in range(CHUNK):
                total = total + e[:, c * tok : (c + 1) * tok]
            return total

        total = lax.fori_loop(0, full + 1, expo, jnp.zeros((2 * tok, tok), jnp.float32))
        total = 1.0 / jnp.sum(total, axis=-1, keepdims=True)
        one, two = total[:tok], total[tok:] * lam

        def mix(j, o):
            p = (sc[j, :tok, :] * one - sc[j, tok:, :] * two).astype(jnp.bfloat16)
            return o + jnp.dot(
                p, vall[pl.ds(pl.multiple_of(j * span, span), span), :],
                preferred_element_type=jnp.float32,
            )

        o = lax.fori_loop(0, full + 1, mix, jnp.zeros((tok, vall.shape[1]), jnp.float32))
        o = o * lax.rsqrt(jnp.mean(o * o, axis=-1, keepdims=True) + EPSILON)
        return (o * hg_ref[...] * OUT_SCALE).astype(jnp.bfloat16)

    for which in range(3):
        own(which).wait()

    w_on_turn = jnp.where(is_lead, n // 16, (3 * n) // 8)
    w_rest_turn = jnp.where(is_lead, n // 2, jnp.where(me < n // 2, (3 * n) // 4, n - 1))

    def turn(s, c):
        @pl.when(s == w_on_turn)
        def _():
            w_on()

        @pl.when(s == w_rest_turn)
        def _():
            w_rest()

        number = s

        @pl.when(number != me)
        def _():
            for which in range(3):
                chunk_arrived(which, number)

        rows = pl.ds(pl.multiple_of(number * tok, tok), tok)
        krot[rows, :] = rotate(kraw[number], number, gains[1:2, :])
        vall[rows, :] = vraw[number]

        o = attend(number)

        @pl.when(number == me)
        def _():
            oin[:, pl.ds(pl.multiple_of(me * tok, tok), tok)] = o

        @pl.when(number != me)
        def _():
            osend[number] = o
            chunk_copy(3, number).start()

        return c

    lax.fori_loop(0, n, turn, 0)
    own_w.wait()
    for chips, way in p_list:
        p_arrived(chips, way)

    acc[...] = jnp.zeros_like(acc)
    groups = n // CHUNK

    def head_group(turn, c):
        g = lax.rem(turn + first, groups)
        for j in range(CHUNK):
            block = g * CHUNK + j

            @pl.when(block != me)
            def _():
                chunk_arrived(3, block)

        cols = pl.ds(pl.multiple_of(g * span, span), span)
        acc[...] += jnp.dot(oin[:, cols], w_all[cols, :], preferred_element_type=jnp.float32)
        return c

    lax.fori_loop(0, groups, head_group, 0)
    out_ref[0] = acc[...].astype(jnp.bfloat16)

    def sent(p, c):
        @pl.when(p != me)
        def _():
            for which in range(4):
                chunk_copy(which, p).wait_send()

        return c

    lax.fori_loop(0, n, sent, 0)
    for phase in (0, 1):
        for k, way, d in along:
            w_copy(phase, k, way, d).wait_send()
    for chips, way in p_list:
        p_copy(chips, way).wait_send()


def local(query_rows, key_rows, value_rows, query_gain, key_gain, lambdas, head_gain, out_weight):
    n, nd = lax.axis_size("sp"), lax.axis_size("dp")
    head, vdim = query_gain.shape[0], head_gain.shape[0]
    _, tok, total = query_rows.shape
    lanes = 2 * head
    assert lambdas.shape[0] == n and total == n * lanes and vdim == lanes and tok == vdim
    table = rope_tables(n, tok, head)
    columns = out_weight.shape[1] * nd
    reach = max(nd // 8, 1)
    anywhere = pl.BlockSpec(memory_space=pl.ANY)
    vmem = pl.BlockSpec(memory_space=pltpu.VMEM)
    smem = pl.BlockSpec(memory_space=pltpu.SMEM)
    dma = pltpu.SemaphoreType.DMA
    bf16, f32 = jnp.bfloat16, jnp.float32
    return pl.pallas_call(
        functools.partial(kernel, n, nd, head),
        out_shape=jax.ShapeDtypeStruct((1, tok, columns), bf16),
        in_specs=[anywhere] * 4 + [vmem, vmem, smem, vmem, vmem],
        out_specs=vmem,
        scratch_shapes=[
            pltpu.VMEM((n, tok, lanes), bf16),
            pltpu.VMEM((n, tok, vdim), bf16),
            pltpu.VMEM((n, tok, lanes), bf16),
            pltpu.VMEM((n * tok, lanes), bf16),
            pltpu.VMEM((n * tok, vdim), bf16),
            pltpu.VMEM((n, tok, vdim), bf16),
            pltpu.VMEM((tok, n * vdim), bf16),
            pltpu.VMEM((n * vdim, columns), bf16),
            pltpu.VMEM((n // CHUNK, 2 * tok, CHUNK * tok), f32),
            pltpu.VMEM((tok, columns), f32),
            pltpu.VMEM((8, lanes), f32),
            dma((4,)), dma((4, n)), dma((4, n)),
            dma((2 * reach, 2)), dma((2 * reach, 2)),
            dma((2 * reach + 1, 2)), dma((2 * reach + 1, 2)),
            pltpu.SemaphoreType.REGULAR((n,)), pltpu.SemaphoreType.REGULAR,
        ],
        compiler_params=pltpu.CompilerParams(
            collective_id=0, has_side_effects=True, vmem_limit_bytes=67_043_328
        ),
    )(
        query_rows, key_rows, value_rows, out_weight,
        query_gain.reshape(1, head), key_gain.reshape(1, head), lambdas,
        head_gain.reshape(1, vdim), jnp.asarray(table),
    )


def solution(mesh):
    placed = (
        P(("grp", "dp"), "sp", None),
        P(("grp", "dp"), "sp", None),
        P(("grp", "dp"), "sp", None),
        P(),
        P(),
        P(),
        P(),
        P(None, "dp"),
    )
    return jax.shard_map(
        local, mesh=mesh, in_specs=placed, out_specs=P(("grp", "dp"), "sp", None), check_vma=False
    )
```

```python
import functools

import jax
import jax.numpy as jnp
import numpy as np
from jax import lax
from jax.experimental import pallas as pl
from jax.experimental.pallas import tpu as pltpu
from jax.sharding import PartitionSpec as P

EPSILON = 1e-06
OUT_SCALE = 0.8
LOG2E = 1.4426950408889634
NEG = -1e30
MESH = pl.DeviceIdType.MESH
CHUNK = 4


def rope_tables(blocks, block, head):
    half = head // 2
    lane = np.arange(2 * head) % head
    inverse = 10000.0 ** (-(lane % half).astype(np.float64) / half)
    sign = np.where(lane < half, -1.0, 1.0)

    def pair(positions):
        angle = positions[:, None] * inverse[None, :]
        return np.stack([np.cos(angle), sign * np.sin(angle)]).astype(np.float32)

    return np.concatenate(
        [pair(np.arange(blocks) * float(block)), pair(np.arange(block).astype(np.float64))], axis=1
    )


def kernel(
    n, nd, head,
    q_hbm, k_hbm, v_hbm, w_hbm, qg_ref, kg_ref, lam_ref, hg_ref, table_ref,
    out_ref,
    kraw, vraw, qraw, krot, vall, osend, oin, w_all, sc, acc, gains,
    loc_sem, send_sem, recv_sem, wsend, wrecv, psend, precv, ready, lead_in,
):
    me = lax.axis_index("sp")
    dp = lax.axis_index("dp")
    lead_ring = (dp == 0) & (lax.axis_index("grp") == 0)
    lead_plane = (me == 0) & (lax.axis_index("grp") == 0)
    is_lead = lead_ring & lead_plane
    core = lax.rem(dp, 2)
    partner = dp + 1 - 2 * core
    reach = max(nd // 8, 1)
    along = [
        (k, way, lax.rem(dp + (2 * k if way == 0 else nd - 2 * k), nd))
        for k in range(1, reach + 1)
        for way in (0, 1)
    ]
    beside = [d for _, _, d in along] + [partner]
    tok = out_ref.shape[1]
    depth, width = w_hbm.shape
    lanes = 2 * head

    first = jnp.where(lead_ring, 1, 0)
    pos = lax.rem(me - first + n, n)

    def at(p):
        return lax.rem(p + first, n)

    def leads(d):
        return lead_plane & (d == 0)

    beside_lead = sum(leads(d).astype(jnp.int32) for d in beside)

    def enter():
        sem = pltpu.get_barrier_semaphore()

        @pl.when(jnp.logical_not(is_lead))
        def _():
            for d in beside:
                pl.semaphore_signal(sem, inc=1, device_id={"dp": d}, device_id_type=MESH)

        pl.semaphore_wait(sem, len(beside) - beside_lead + jnp.where(pos > 0, 1, 0))

        @pl.when(pos < n - 1)
        def _():
            pl.semaphore_signal(sem, inc=1, device_id={"sp": at(pos + 1)}, device_id_type=MESH)

        @pl.when(is_lead)
        def _():
            for d in beside:
                pl.semaphore_signal(lead_in, inc=1, device_id={"dp": d}, device_id_type=MESH)

        def tell(p, c):
            pl.semaphore_signal(ready.at[me], inc=1, device_id={"sp": at(p)}, device_id_type=MESH)
            return c

        lax.fori_loop(0, pos, tell, 0)

    raws = (kraw, vraw, qraw)

    def chunk_copy(which, peer):
        if which == 3:
            src = osend.at[peer]
            dst = oin.at[:, pl.ds(pl.multiple_of(me * tok, tok), tok)]
        else:
            src = (k_hbm, v_hbm, q_hbm)[which].at[
                0, :, pl.ds(pl.multiple_of(peer * lanes, lanes), lanes)
            ]
            dst = raws[which].at[me]
        return pltpu.make_async_remote_copy(
            src_ref=src, dst_ref=dst,
            send_sem=send_sem.at[which, peer], recv_sem=recv_sem.at[which, me],
            device_id={"sp": peer}, device_id_type=MESH,
        )

    def chunk_arrived(which, peer):
        if which == 3:
            dst = oin.at[:, pl.ds(pl.multiple_of(peer * tok, tok), tok)]
        else:
            dst = raws[which].at[peer]
        pltpu.make_async_remote_copy(
            src_ref=dst, dst_ref=dst,
            send_sem=send_sem.at[which, peer], recv_sem=recv_sem.at[which, peer],
            device_id={"sp": peer}, device_id_type=MESH,
        ).wait_recv()

    def own(which):
        cols = pl.ds(pl.multiple_of(me * lanes, lanes), lanes)
        return pltpu.make_async_copy(
            (k_hbm, v_hbm, q_hbm)[which].at[0, :, cols], raws[which].at[me], loc_sem.at[which]
        )

    def w_at(owner, lo=0, rows=None):
        rows = depth if rows is None else rows
        return w_all.at[pl.ds(lo, rows), pl.ds(pl.multiple_of(owner * width, width), width)]

    half = depth // 2

    def away(device, chips, way):
        return lax.rem(device + (nd - 2 * chips if way == 0 else 2 * chips), nd)

    def remote(src, dst, send, recv, d):
        return pltpu.make_async_remote_copy(
            src_ref=src, dst_ref=dst, send_sem=send, recv_sem=recv,
            device_id={"dp": d}, device_id_type=MESH,
        )

    def w_part(phase, k, way):
        if phase == 0 or k < reach:
            return 0, depth
        return (0, half) if way == 0 else (half, half)

    def w_copy(phase, k, way, d):
        dst = w_at(away(dp, phase * k, way), *w_part(phase, k, way))
        i = phase * reach + k - 1
        return remote(w_hbm if phase == 0 else dst, dst, wsend.at[i, way], wrecv.at[i, way], d)

    def w_arrived(phase, k, way):
        dst = w_at(away(dp, k + phase * reach, way), *w_part(phase, k, way))
        i = phase * reach + k - 1
        remote(dst, dst, wsend.at[i, way], wrecv.at[i, way], partner).wait_recv()

    p_list = [(0, 0)] + [(c, way) for c in range(1, 2 * reach) for way in (0, 1)] + [(2 * reach, 0)]

    def p_copy(chips, way):
        dst = w_at(away(dp, chips, way))
        return remote(
            w_hbm if chips == 0 else dst, dst, psend.at[chips, way], precv.at[chips, way], partner
        )

    def p_arrived(chips, way):
        dst = w_at(away(partner, chips, way))
        remote(dst, dst, psend.at[chips, way], precv.at[chips, way], partner).wait_recv()

    def w_first(to_lead):
        copies = [(w_copy(0, k, way, d), d) for k, way, d in along] + [(p_copy(0, 0), partner)]
        for copy, d in copies:

            @pl.when(leads(d) if to_lead else jnp.logical_not(leads(d)))
            def _():
                copy.start()

    far = [d for k, _, d in along if k == reach]

    def w_on():
        for k in range(1, reach + 1):
            for way in (0, 1):
                w_arrived(0, k, way)
                w_copy(1, k, way, far[way]).start()
                p_copy(k, way).start()

    def w_rest():
        for k in range(1, reach + 1):
            for way in (0, 1):
                w_arrived(1, k, way)
                if k < reach:
                    p_copy(reach + k, way).start()
        p_copy(2 * reach, 0).start()

    for which in range(3):
        own(which).start()
    own_w = pltpu.make_async_copy(w_hbm, w_at(dp), loc_sem.at[3])
    own_w.start()
    enter()

    def send_to(p):
        for which in range(3):
            chunk_copy(which, at(p)).start()

    wraps = jnp.maximum(jnp.where(lead_ring & (pos > n // 2), n, pos - n // 2), 0)

    near = (3 * n) // 8
    holds = (pos > n // 2) & jnp.logical_not(lead_ring)

    def held(p):
        return holds & (pos - p > near) & (pos - p <= n // 2)

    def send_held(k, c):
        send_to(pos - k)
        return c

    def send_lower(s, c):
        down = jnp.where(s < 2 * wraps, s // 2, s - wraps)
        turned = (s < 2 * wraps) & (lax.rem(s, 2) == 1)
        p = jnp.where(turned, s // 2, pos - 1 - down)

        @pl.when(jnp.logical_not(held(p)))
        def _():
            send_to(p)

        return c

    def send_upper(p, c):
        pl.semaphore_wait(ready.at[at(p)], 1)
        send_to(p)
        return c

    w_first(False)
    lax.fori_loop(0, pos, send_lower, 0)
    ahead = jnp.where(lead_ring, (3 * n) // 4 + 1, n)
    lax.fori_loop(pos + 1, jnp.maximum(pos + 1, ahead), send_upper, 0)

    @pl.when(jnp.logical_not(is_lead) & (beside_lead > 0))
    def _():
        pl.semaphore_wait(lead_in, beside_lead)
        w_first(True)


    for row, ref in ((0, qg_ref), (1, kg_ref)):
        g = ref[...]
        gains[row : row + 1, :] = jnp.concatenate([g, g], axis=1)
    lane = lax.broadcasted_iota(jnp.int32, (1, lanes), 1)
    low_half = lax.rem(lane, head) < head // 2
    first_map = lane < head
    ri = lax.broadcasted_iota(jnp.int32, (lanes, lanes), 0) // head
    ci = lax.broadcasted_iota(jnp.int32, (lanes, lanes), 1) // head
    ones = (ri == ci).astype(jnp.float32).astype(jnp.bfloat16)
    krot[...] = jnp.zeros_like(krot)
    vall[...] = jnp.zeros_like(vall)

    def rotate(raw, number, gain):
        x = raw.astype(jnp.float32)
        sq = x * x
        hi = sq.astype(jnp.bfloat16)
        lo = (sq - hi.astype(jnp.float32)).astype(jnp.bfloat16)
        total = jnp.dot(hi, ones, preferred_element_type=jnp.float32) + jnp.dot(
            lo, ones, preferred_element_type=jnp.float32
        )
        y = x * lax.rsqrt(total * (1.0 / head) + EPSILON) * gain
        cb, sb = table_ref[0, pl.ds(number, 1), :], table_ref[1, pl.ds(number, 1), :]
        co, so = table_ref[0, n : n + tok, :], table_ref[1, n : n + tok, :]
        cosine = cb * co - sb * so
        sine = sb * co + cb * so
        other = jnp.where(
            low_half, pltpu.roll(y, lanes - head // 2, 1), pltpu.roll(y, head // 2, 1)
        )
        return (y * cosine + other * sine).astype(jnp.bfloat16)

    lam = lam_ref[me]
    span = CHUNK * tok

    def attend(number):
        q = rotate(qraw[number], number, gains[0:1, :]) * jnp.bfloat16(head**-0.5)
        zero = jnp.zeros_like(q)
        both = jnp.concatenate(
            [jnp.where(first_map, q, zero), jnp.where(first_map, zero, q)], axis=0
        )
        full = number // CHUNK

        def score(j):
            keys = krot[pl.ds(pl.multiple_of(j * span, span), span), :]
            return lax.dot_general(
                both, keys, (((1,), (1,)), ((), ())), preferred_element_type=jnp.float32
            )

        def highest(s, m):
            for c in range(CHUNK):
                m = jnp.maximum(m, s[:, c * tok : (c + 1) * tok])
            return m

        def body(j, m):
            s = score(j)
            sc[j] = s
            return highest(s, m)

        m = lax.fori_loop(0, full, body, jnp.full((2 * tok, tok), NEG, jnp.float32))
        s = score(full)
        row = lax.rem(lax.broadcasted_iota(jnp.int32, s.shape, 0), tok) + number * tok
        col = lax.broadcasted_iota(jnp.int32, s.shape, 1) + full * span
        s = jnp.where(col <= row, s, NEG)
        sc[full] = s
        m = jnp.max(highest(s, m), axis=-1, keepdims=True)

        def expo(j, total):
            e = jnp.exp2((sc[j] - m) * LOG2E)
            sc[j] = e
            for c in range(CHUNK):
                total = total + e[:, c * tok : (c + 1) * tok]
            return total

        total = lax.fori_loop(0, full + 1, expo, jnp.zeros((2 * tok, tok), jnp.float32))
        total = 1.0 / jnp.sum(total, axis=-1, keepdims=True)
        one, two = total[:tok], total[tok:] * lam

        def mix(j, o):
            p = (sc[j, :tok, :] * one - sc[j, tok:, :] * two).astype(jnp.bfloat16)
            return o + jnp.dot(
                p, vall[pl.ds(pl.multiple_of(j * span, span), span), :],
                preferred_element_type=jnp.float32,
            )

        o = lax.fori_loop(0, full + 1, mix, jnp.zeros((tok, vall.shape[1]), jnp.float32))
        o = o * lax.rsqrt(jnp.mean(o * o, axis=-1, keepdims=True) + EPSILON)
        return (o * hg_ref[...] * OUT_SCALE).astype(jnp.bfloat16)

    for which in range(3):
        own(which).wait()

    w_on_turn = jnp.where(is_lead, 0, (3 * n) // 8)
    w_rest_turn = jnp.where(is_lead, n // 16, jnp.where(me < n // 2, (3 * n) // 4, n - 1))

    def turn(s, c):
        @pl.when((s == n // 8) & holds)
        def _():
            lax.fori_loop(near + 1, n // 2 + 1, send_held, 0)

        @pl.when(s == w_on_turn)
        def _():
            w_on()

        @pl.when(s == w_rest_turn)
        def _():
            w_rest()

        number = s

        @pl.when(number != me)
        def _():
            for which in range(3):
                chunk_arrived(which, number)

        rows = pl.ds(pl.multiple_of(number * tok, tok), tok)
        krot[rows, :] = rotate(kraw[number], number, gains[1:2, :])
        vall[rows, :] = vraw[number]

        o = attend(number)

        @pl.when(number == me)
        def _():
            oin[:, pl.ds(pl.multiple_of(me * tok, tok), tok)] = o

        @pl.when(number != me)
        def _():
            osend[number] = o
            chunk_copy(3, number).start()

        upper = jnp.maximum(ahead, pos + 1) + s

        @pl.when(upper < n)
        def _():
            send_upper(upper, 0)

        return c

    lax.fori_loop(0, n, turn, 0)
    own_w.wait()
    for chips, way in p_list:
        p_arrived(chips, way)

    acc[...] = jnp.zeros_like(acc)
    groups = n // CHUNK

    def head_group(turn, c):
        g = lax.rem(turn + first, groups)
        for j in range(CHUNK):
            block = g * CHUNK + j

            @pl.when(block != me)
            def _():
                chunk_arrived(3, block)

        cols = pl.ds(pl.multiple_of(g * span, span), span)
        acc[...] += jnp.dot(oin[:, cols], w_all[cols, :], preferred_element_type=jnp.float32)
        return c

    lax.fori_loop(0, groups, head_group, 0)
    out_ref[0] = acc[...].astype(jnp.bfloat16)

    def sent(p, c):
        @pl.when(p != me)
        def _():
            for which in range(4):
                chunk_copy(which, p).wait_send()

        return c

    lax.fori_loop(0, n, sent, 0)
    for phase in (0, 1):
        for k, way, d in along:
            w_copy(phase, k, way, d).wait_send()
    for chips, way in p_list:
        p_copy(chips, way).wait_send()


def local(query_rows, key_rows, value_rows, query_gain, key_gain, lambdas, head_gain, out_weight):
    n, nd = lax.axis_size("sp"), lax.axis_size("dp")
    head, vdim = query_gain.shape[0], head_gain.shape[0]
    _, tok, total = query_rows.shape
    lanes = 2 * head
    assert lambdas.shape[0] == n and total == n * lanes and vdim == lanes and tok == vdim
    table = rope_tables(n, tok, head)
    columns = out_weight.shape[1] * nd
    reach = max(nd // 8, 1)
    anywhere = pl.BlockSpec(memory_space=pl.ANY)
    vmem = pl.BlockSpec(memory_space=pltpu.VMEM)
    smem = pl.BlockSpec(memory_space=pltpu.SMEM)
    dma = pltpu.SemaphoreType.DMA
    bf16, f32 = jnp.bfloat16, jnp.float32
    return pl.pallas_call(
        functools.partial(kernel, n, nd, head),
        out_shape=jax.ShapeDtypeStruct((1, tok, columns), bf16),
        in_specs=[anywhere] * 4 + [vmem, vmem, smem, vmem, vmem],
        out_specs=vmem,
        scratch_shapes=[
            pltpu.VMEM((n, tok, lanes), bf16),
            pltpu.VMEM((n, tok, vdim), bf16),
            pltpu.VMEM((n, tok, lanes), bf16),
            pltpu.VMEM((n * tok, lanes), bf16),
            pltpu.VMEM((n * tok, vdim), bf16),
            pltpu.VMEM((n, tok, vdim), bf16),
            pltpu.VMEM((tok, n * vdim), bf16),
            pltpu.VMEM((n * vdim, columns), bf16),
            pltpu.VMEM((n // CHUNK, 2 * tok, CHUNK * tok), f32),
            pltpu.VMEM((tok, columns), f32),
            pltpu.VMEM((8, lanes), f32),
            dma((4,)), dma((4, n)), dma((4, n)),
            dma((2 * reach, 2)), dma((2 * reach, 2)),
            dma((2 * reach + 1, 2)), dma((2 * reach + 1, 2)),
            pltpu.SemaphoreType.REGULAR((n,)), pltpu.SemaphoreType.REGULAR,
        ],
        compiler_params=pltpu.CompilerParams(
            collective_id=0, has_side_effects=True, vmem_limit_bytes=67_043_328
        ),
    )(
        query_rows, key_rows, value_rows, out_weight,
        query_gain.reshape(1, head), key_gain.reshape(1, head), lambdas,
        head_gain.reshape(1, vdim), jnp.asarray(table),
    )


def solution(mesh):
    placed = (
        P(("grp", "dp"), "sp", None),
        P(("grp", "dp"), "sp", None),
        P(("grp", "dp"), "sp", None),
        P(),
        P(),
        P(),
        P(),
        P(None, "dp"),
    )
    return jax.shard_map(
        local, mesh=mesh, in_specs=placed, out_specs=P(("grp", "dp"), "sp", None), check_vma=False
    )
```
